32 devices in a mesh: fs: 8 (over z, x), tp: 4 (over y, core).
Axes of the slice: x: 2, y: 2, z: 4, core: 2. Of those that a mesh axis runs over, the one named last changes fastest.
Arguments:
- weights: float32 [2, 5632, 2048], P(None, 'fs', 'tp'), may hold values from -6 to 6
- momentum: float32 [2, 5632, 2048], P(None, 'fs', 'tp'), may hold values from -12 to 12
- gradients: float32 [2, 5632, 2048], P(None, 'fs', 'tp'), may hold values from -140 to 140
Outputs:
- new_weights: float32 [2, 5632, 2048], P(None, 'fs', 'tp')
- new_momentum: float32 [2, 5632, 2048], P(None, 'fs', 'tp')
- update: float32 [2, 5632, 2048], P(None, 'fs', 'tp')
The draws below stay inside these ranges and needn't reach their ends.
All inputs are finite; a program needn't handle non-finite values.
Results may differ from the reference program's by a relative error of at most 0.035.
Values may be sent and summed in bfloat16 or wider, within the bound.
A program may use at most 64 MiB of HBM per device.

```python
import math
import jax
import jax.numpy as jnp
from jax import lax

D = 2048
FF = 5632
MATS = 2
ITERS = 3


def draw_gradients(key, part):
    key_noise, key_rows, key_cols = jax.random.split(key, 3)
    row_ramp = jnp.arange(FF, dtype=jnp.float32) / FF
    col_ramp = jnp.arange(D, dtype=jnp.float32) / D
    row_jitter = jax.random.uniform(key_rows, (MATS, FF, 1), jnp.float32, 0.85, 1.15)
    col_jitter = jax.random.uniform(key_cols, (MATS, 1, D), jnp.float32, 0.9, 1.1)
    row_scale = jnp.power(1.75, row_ramp)[None, :, None] * row_jitter
    col_scale = jnp.power(6.0, col_ramp)[None, None, :] * col_jitter
    noise_draw = jax.random.truncated_normal(key_noise, -4.0, 4.0, (MATS, FF, D), jnp.float32)
    values = 2.5 * noise_draw * row_scale * col_scale
    return values.astype(jnp.float32)


def steps_of(stream_key, extent, cuts, least, high):
    loudness, own = 1.0, jax.random.fold_in(stream_key, 6)
    for axis_at, blocks in cuts:
        draws = jnp.exp(jax.random.uniform(jax.random.fold_in(own, axis_at), (blocks,), jnp.float32, least / len(cuts), high / len(cuts)))
        loudness = loudness * jnp.repeat(draws, extent[axis_at] // blocks).reshape([-1 if axis == axis_at else 1 for axis in range(len(extent))])
    return loudness


def centred(stream_key, shape, width, reach, cuts=(), held_as=jnp.bfloat16):
    factor_of = steps_of(stream_key, shape, cuts, -0.22, 0.18) if cuts else 1.0
    entries = jax.random.normal(stream_key, shape, jnp.float32) * width * factor_of
    return jnp.minimum(jnp.maximum(entries, -reach), reach).astype(held_as)


def setup_inputs(seed: int = 0) -> dict:
    keys = jax.random.split(jax.random.key(seed), 4)
    return {
        "weights": centred(keys[0], (MATS, FF, D), 1.0, 6.0, ((1, 8), (2, 4)), jnp.float32),
        "momentum": centred(keys[1], (MATS, FF, D), 2.0, 12.0, ((1, 8), (2, 4)), jnp.float32),
        "gradients": draw_gradients(jax.random.fold_in(keys[3], 71), 0),
    }


MOMENTUM_DECAY = 0.95
FIRST_COEF = 3.4445
SECOND_COEF = -4.775
THIRD_COEF = 2.0315
LEARN_RATE = 0.02
WEIGHT_DECAY = 0.1
EPSILON = 1e-07
STEP_SCALE = 0.2
NORM_SAFETY = 1.8

def reference(weights, momentum, gradients):
    new_momentum = MOMENTUM_DECAY * momentum + gradients
    iterate = gradients + MOMENTUM_DECAY * new_momentum
    for step in range(ITERS):
        plain = iterate.astype(jnp.bfloat16)
        plain_wide = plain.astype(jnp.float32)
        gram = jnp.einsum('prj,prk->pjk', plain_wide, plain_wide, precision=lax.Precision.HIGHEST)
        gram_bf = gram.astype(jnp.bfloat16)
        gram_wide = gram_bf.astype(jnp.float32)
        if step == 0:
            squares = lax.optimization_barrier(jnp.sum(gram * gram, axis=(1, 2)))
            ratio = (1.0 / (NORM_SAFETY * jnp.sqrt(jnp.sqrt(squares / D)) + EPSILON))[:, None, None]
        else:
            ratio = 1.0
        cubed = jnp.einsum('prk,pkj->prj', plain_wide, gram_wide, precision=lax.Precision.HIGHEST)
        cubed = (cubed * ratio ** 3).astype(jnp.bfloat16)
        folded = jnp.einsum('prk,pkj->prj', cubed.astype(jnp.float32), gram_wide, precision=lax.Precision.HIGHEST)
        iterate = FIRST_COEF * ratio * iterate + SECOND_COEF * cubed.astype(jnp.float32) + THIRD_COEF * (ratio * ratio) * folded
    update = STEP_SCALE * math.sqrt(max(FF, D)) * iterate
    new_weights = weights * (1.0 - LEARN_RATE * WEIGHT_DECAY) - LEARN_RATE * update
    return (new_weights, new_momentum, update)
```

```python
import functools
import math

import jax
import jax.numpy as jnp
from jax import lax
from jax.experimental import pallas as pl
from jax.experimental.pallas import tpu as pltpu
from jax.sharding import Mesh, PartitionSpec as P

MOMENTUM_DECAY = 0.95
FIRST_COEF = 3.4445
SECOND_COEF = -4.775
THIRD_COEF = 2.0315
LEARN_RATE = 0.02
WEIGHT_DECAY = 0.1
EPSILON = 1e-07
STEP_SCALE = 0.2
NORM_SAFETY = 1.8
ITERS = 3

BLOCKS = 8
KEPT = BLOCKS // 2 + 1


def mm(a, b):
    return jnp.dot(a, b, preferred_element_type=jnp.float32)


def polar_kernel(scale_ref, wedge_ref, rows_ref, out_ref, gram, poly, half, wide):
    width = gram.shape[0]
    size = width // BLOCKS
    for i in range(BLOCKS):
        for k in range(KEPT):
            j = (i + k) % BLOCKS
            block = wedge_ref[i, :, k * size : (k + 1) * size]
            gram[i * size : (i + 1) * size, j * size : (j + 1) * size] = block
            if 0 < k < KEPT - 1:
                gram[j * size : (j + 1) * size, i * size : (i + 1) * size] = block.T

    ratio = scale_ref[0]
    square = scale_ref[1]
    tile = min(512, width)
    per_row = width // tile

    def over_tiles(body):
        def step(t, carry):
            i, j = t // per_row, t % per_row
            body(pl.ds(pl.multiple_of(i * tile, tile), tile), pl.ds(pl.multiple_of(j * tile, tile), tile))
            return carry

        lax.fori_loop(0, per_row * per_row, step, 0)

    for step in range(ITERS):
        unit = square if step == 0 else 1.0

        def to_poly(r, c):
            product = mm(gram[r, :], gram[:, c])
            mix = SECOND_COEF * gram[r, c].astype(jnp.float32) + (THIRD_COEF * unit) * product
            poly[r, c] = (unit * mix).astype(jnp.bfloat16)

        over_tiles(to_poly)

        def to_rows(t, carry):
            c = pl.ds(pl.multiple_of(t * tile, tile), tile)
            if step == 0:
                held = rows_ref[:, c].astype(jnp.float32)
                fresh = ratio * (FIRST_COEF * held + mm(rows_ref[...], poly[:, c]))
            else:
                fresh = FIRST_COEF * wide[:, c] + mm(out_ref[...], poly[:, c])
            wide[:, c] = fresh
            return carry

        lax.fori_loop(0, per_row, to_rows, 0)
        out_ref[...] = wide[...].astype(jnp.bfloat16)

        if step < ITERS - 1:

            def to_half(r, c):
                product = mm(gram[r, :], poly[:, c])
                half[r, c] = (unit * (FIRST_COEF * gram[r, c].astype(jnp.float32) + product)).astype(jnp.bfloat16)

            over_tiles(to_half)

            def to_gram(r, c):
                product = mm(half[r, :], poly[:, c])
                gram[r, c] = (FIRST_COEF * half[r, c].astype(jnp.float32) + product).astype(jnp.bfloat16)

            over_tiles(to_gram)


def polar(scales, wedge, rows):
    width = rows.shape[1]
    vmem = pl.BlockSpec(memory_space=pltpu.VMEM)
    return pl.pallas_call(
        polar_kernel,
        out_shape=jax.ShapeDtypeStruct(rows.shape, jnp.bfloat16),
        in_specs=[pl.BlockSpec(memory_space=pltpu.SMEM), vmem, vmem],
        out_specs=vmem,
        scratch_shapes=[
            pltpu.VMEM((width, width), jnp.bfloat16),
            pltpu.VMEM((width, width), jnp.bfloat16),
            pltpu.VMEM((width, width), jnp.bfloat16),
            pltpu.VMEM(rows.shape, jnp.float32),
        ],
        compiler_params=pltpu.CompilerParams(vmem_limit_bytes=56 * 1024 * 1024),
    )(scales, wedge, rows)


def per_device(subs, weights, momentum, gradients):
    mats, deep, narrow = gradients.shape
    width = narrow * mats * subs
    part = deep // subs
    new_momentum = MOMENTUM_DECAY * momentum + gradients
    plain = (gradients + MOMENTUM_DECAY * new_momentum).astype(jnp.bfloat16)

    pieces = plain.reshape(mats * subs, part, narrow)
    pieces = lax.all_to_all(pieces, ("mat", "sub"), 0, 0, tiled=True)
    rows = pieces.transpose(1, 0, 2).reshape(part, width)
    whole = lax.all_gather(rows, "sub", axis=0, tiled=True)

    size = width // BLOCKS
    own = BLOCKS // subs
    start = lax.axis_index("sub") * (own * size)
    turned = lax.dynamic_slice_in_dim(jnp.concatenate([whole, whole], axis=1), start, width, axis=1)
    partial_value = jnp.stack(
        [
            lax.dot_general(
                turned[:, b * size : (b + 1) * size],
                turned[:, b * size : (b + KEPT) * size],
                (((0,), (0,)), ((), ())),
                preferred_element_type=jnp.float32,
            ).astype(jnp.bfloat16)
            for b in range(own)
        ]
    )
    share = lax.psum_scatter(partial_value, "fs", scatter_dimension=1, tiled=True)
    wedge = lax.all_gather(share, "fs", axis=1, tiled=True)
    wedge = lax.all_gather(wedge, "sub", axis=0, tiled=True)

    by_block = jnp.sum(jnp.square(wedge.astype(jnp.float32)).reshape(BLOCKS * size, KEPT, size), axis=(0, 2))
    squares = 2.0 * jnp.sum(by_block) - by_block[0] - by_block[KEPT - 1]
    ratio = 1.0 / (NORM_SAFETY * jnp.sqrt(jnp.sqrt(squares / width)) + EPSILON)
    rows = polar(jnp.stack([ratio, ratio * ratio]), wedge, rows)

    pieces = rows.reshape(part, mats * subs, narrow).transpose(1, 0, 2)
    pieces = lax.all_to_all(pieces, ("mat", "sub"), 0, 0, tiled=True)
    iterate = pieces.reshape(mats, deep, narrow).astype(jnp.float32)
    deepest = deep * lax.axis_size("fs")
    update = STEP_SCALE * math.sqrt(max(deepest, width)) * iterate
    new_weights = weights * (1.0 - LEARN_RATE * WEIGHT_DECAY) - LEARN_RATE * update
    return (new_weights, new_momentum, update)


def solution(mesh):
    depth, tp = mesh.devices.shape
    mats = 2
    subs = tp // mats
    fine = Mesh(mesh.devices.reshape(depth, mats, subs), ("fs", "mat", "sub"))
    spec = P(None, "fs", ("mat", "sub"))
    return jax.shard_map(
        functools.partial(per_device, subs),
        mesh=fine,
        in_specs=(spec, spec, spec),
        out_specs=(spec, spec, spec),
        check_vma=False,
    )
```

```python
import functools
import math

import jax
import jax.numpy as jnp
from jax import lax
from jax.experimental import pallas as pl
from jax.experimental.pallas import tpu as pltpu
from jax.sharding import Mesh, PartitionSpec as P

MOMENTUM_DECAY = 0.95
FIRST_COEF = 3.4445
SECOND_COEF = -4.775
THIRD_COEF = 2.0315
LEARN_RATE = 0.02
WEIGHT_DECAY = 0.1
EPSILON = 1e-07
STEP_SCALE = 0.2
NORM_SAFETY = 1.8
ITERS = 3

BLOCKS = 8
NEAR = BLOCKS // 2


def mm(a, b):
    return jnp.dot(a, b, preferred_element_type=jnp.float32)


def polar_kernel(subs, wedge_ref, rows_ref, out_ref, gram, poly, half, wide, tally):
    width = gram.shape[0]
    size = width // BLOCKS
    own = BLOCKS // subs
    per_sub = wedge_ref.shape[0] // subs

    def place(at, i, j, weight):
        block = wedge_ref[at]
        r = pl.ds(pl.multiple_of(i * size, size), size)
        c = pl.ds(pl.multiple_of(j * size, size), size)
        gram[r, c] = block
        if weight > 1.0:
            gram[c, r] = block.T
        full = block.astype(jnp.float32)
        tally[...] += weight * jnp.sum(full * full, axis=0, keepdims=True)

    tally[...] = jnp.zeros_like(tally)

    def place_row(i, carry):
        base = (i // own) * per_sub + (i % own) * NEAR
        for k in range(NEAR):
            place(base + k, i, (i + k) % BLOCKS, 1.0 if k == 0 else 2.0)
        return carry

    lax.fori_loop(0, BLOCKS, place_row, 0)
    for s in range(subs):
        for m in range(own // 2):
            i = s * own + m + (own // 2 if 2 * s >= subs else 0)
            place(s * per_sub + own * NEAR + m, i, (i + NEAR) % BLOCKS, 2.0)

    squares = jnp.sum(tally[...], axis=1, keepdims=True)
    first_ratio = 1.0 / (NORM_SAFETY * jnp.sqrt(jnp.sqrt(squares / width)) + EPSILON)
    wide[...] = rows_ref[...].astype(jnp.float32)
    out_ref[...] = rows_ref[...]
    tile = min(512, width)
    n = width // tile
    apart = n * (n - 1) // 2

    def spot(t):
        i = jnp.where(t < apart, t % n, t - apart)
        j = (i + jnp.where(t < apart, 1 + t // n, 0)) % n
        return pl.ds(pl.multiple_of(i * tile, tile), tile), pl.ds(pl.multiple_of(j * tile, tile), tile)

    def symmetric(target, tile_of):
        def step(t, carry):
            past_r, past_c = spot(jnp.maximum(t - 1, 0))
            target[past_c, past_r] = target[past_r, past_c].T
            r, c = spot(t)
            target[r, c] = tile_of(r, c).astype(jnp.bfloat16)
            return carry

        lax.fori_loop(0, apart + n, step, 0)

    def poly_and_rows(ratio):
        unit = ratio * ratio

        def poly_tile(r, c):
            return unit * (SECOND_COEF * gram[r, c].astype(jnp.float32) + (THIRD_COEF * unit) * mm(gram[r, :], gram[:, c]))

        symmetric(poly, poly_tile)

        def to_rows(t, carry):
            c = pl.ds(pl.multiple_of(t * tile, tile), tile)
            wide[:, c] = ratio * (FIRST_COEF * wide[:, c] + mm(out_ref[...], poly[:, c]))
            return carry

        lax.fori_loop(0, n, to_rows, 0)
        out_ref[...] = wide[...].astype(jnp.bfloat16)

    def full_step(step, carry):
        ratio = jnp.where(step == 0, first_ratio, 1.0)
        unit = ratio * ratio
        poly_and_rows(ratio)
        symmetric(half, lambda r, c: unit * (FIRST_COEF * gram[r, c].astype(jnp.float32) + mm(gram[r, :], poly[:, c])))
        symmetric(gram, lambda r, c: FIRST_COEF * half[r, c].astype(jnp.float32) + mm(half[r, :], poly[:, c]))
        return carry

    lax.fori_loop(0, ITERS - 1, full_step, 0)
    poly_and_rows(jnp.ones_like(first_ratio))


def polar(subs, wedge, rows):
    width = rows.shape[1]
    vmem = pl.BlockSpec(memory_space=pltpu.VMEM)
    return pl.pallas_call(
        functools.partial(polar_kernel, subs),
        out_shape=jax.ShapeDtypeStruct(rows.shape, jnp.bfloat16),
        in_specs=[vmem, vmem],
        out_specs=vmem,
        scratch_shapes=[
            pltpu.VMEM((width, width), jnp.bfloat16),
            pltpu.VMEM((width, width), jnp.bfloat16),
            pltpu.VMEM((width, width), jnp.bfloat16),
            pltpu.VMEM(rows.shape, jnp.float32),
            pltpu.VMEM((1, width // BLOCKS), jnp.float32),
        ],
        compiler_params=pltpu.CompilerParams(vmem_limit_bytes=56 * 1024 * 1024),
    )(wedge, rows)


def per_device(subs, weights, momentum, gradients):
    mats, deep, narrow = gradients.shape
    width = narrow * mats * subs
    part = deep // subs
    new_momentum = MOMENTUM_DECAY * momentum + gradients
    plain = (gradients + MOMENTUM_DECAY * new_momentum).astype(jnp.bfloat16)

    pieces = plain.reshape(mats * subs, part, narrow)
    pieces = lax.all_to_all(pieces, ("mat", "sub"), 0, 0, tiled=True)
    rows = pieces.transpose(1, 0, 2).reshape(part, width)
    whole = lax.all_gather(rows, "sub", axis=0, tiled=True)

    size = width // BLOCKS
    own = BLOCKS // subs
    sub = lax.axis_index("sub")
    start = sub * (own * size)
    turned = lax.dynamic_slice_in_dim(jnp.concatenate([whole, whole], axis=1), start, width, axis=1)

    def product(left, right):
        full = lax.dot_general(left, right, (((0,), (0,)), ((), ())), preferred_element_type=jnp.float32)
        full = full.astype(jnp.bfloat16)
        return [full[:, at : at + size] for at in range(0, full.shape[1], size)]

    blocks = []
    for b in range(own):
        blocks += product(turned[:, b * size : (b + 1) * size], turned[:, b * size : (b + NEAR) * size])
    far = jnp.where(2 * sub >= subs, (own // 2) * size, 0)
    for m in range(own // 2):
        left = lax.dynamic_slice_in_dim(turned, far + m * size, size, axis=1)
        right = lax.dynamic_slice_in_dim(turned, far + (m + NEAR) * size, size, axis=1)
        blocks += product(left, right)
    share = lax.psum_scatter(jnp.stack(blocks), "fs", scatter_dimension=1, tiled=True)
    wedge = lax.all_gather(share, "fs", axis=1, tiled=True)
    wedge = lax.all_gather(wedge, "sub", axis=0, tiled=True)
    rows = polar(subs, wedge, rows)

    pieces = rows.reshape(part, mats * subs, narrow).transpose(1, 0, 2)
    pieces = lax.all_to_all(pieces, ("mat", "sub"), 0, 0, tiled=True)
    iterate = pieces.reshape(mats, deep, narrow).astype(jnp.float32)
    deepest = deep * lax.axis_size("fs")
    update = STEP_SCALE * math.sqrt(max(deepest, width)) * iterate
    new_weights = weights * (1.0 - LEARN_RATE * WEIGHT_DECAY) - LEARN_RATE * update
    return (new_weights, new_momentum, update)


def solution(mesh):
    depth, tp = mesh.devices.shape
    mats = 2
    subs = tp // mats
    fine = Mesh(mesh.devices.reshape(depth, mats, subs), ("fs", "mat", "sub"))
    spec = P(None, "fs", ("mat", "sub"))
    return jax.shard_map(
        functools.partial(per_device, subs),
        mesh=fine,
        in_specs=(spec, spec, spec),
        out_specs=(spec, spec, spec),
        check_vma=False,
    )
```
